32 devices in a mesh: sp: 4 (over z), fs: 4 (over y, x), tp: 2 (over core).
Axes of the slice: x: 2, y: 2, z: 4, core: 2. Of those that a mesh axis runs over, the one named last changes fastest.
Arguments:
- tokens: bfloat16 [4, 512, 4096], P('fs', 'sp', 'tp'), may hold values from -6 to 6
- norm_gain: float32 [4096], replicated, may hold values from 0.1 to 1.9
- w_state_in: bfloat16 [4096, 2048], P(('sp', 'fs'), 'tp'), may hold values from -0.09375 to 0.09375
- w_query: bfloat16 [4096, 2048], P(('sp', 'fs'), 'tp'), may hold values from -0.3125 to 0.3125
- w_key: bfloat16 [4096, 2048], P(('sp', 'fs'), 'tp'), may hold values from -0.3125 to 0.3125
- w_value: bfloat16 [4096, 2048], P(('sp', 'fs'), 'tp'), may hold values from -0.09375 to 0.09375
- decay_re: float32 [128, 64], P('tp'), may hold values from -0.034 to -9.765625e-05
- decay_im: float32 [128, 64], P('tp'), may hold values from -3.140625 to 3.140625
- log_step: float32 [128], P('tp'), may hold values from -3.5 to -1.5
- decay_shift: float32 [4, 128, 512], P('fs', 'tp', 'sp'), may hold values from -2 to 0
- in_re: float32 [128, 64, 16], P('tp'), may hold values from -2 to 2
- in_im: float32 [128, 64, 16], P('tp'), may hold values from -2 to 2
- output_real: float32 [128, 16, 64], P('tp'), may hold values from -0.75 to 0.75
- output_imaginary: float32 [128, 16, 64], P('tp'), may hold values from -0.75 to 0.75
- skip: float32 [2048], P('tp'), may hold values from -1.2 to 1.2
- mix_weight: float32 [8], P('tp'), may hold values from 0.3 to 0.8
- head_gain: float32 [256], replicated, may hold values from 0.1 to 1.9
- w_out_state: bfloat16 [2048, 4096], P('tp'), may hold values from -0.125 to 0.125
- w_out_attn: bfloat16 [2048, 4096], P('tp'), may hold values from -0.125 to 0.125
Outputs:
- mixed: bfloat16 [4, 512, 4096], P('fs', ('sp', 'tp'))
- log_totals: float32 [4, 8, 2, 512], P('fs', 'tp', None, 'sp')
The draws below stay inside these ranges and needn't reach their ends.
All inputs are finite; a program needn't handle non-finite values.
Results may differ from the reference program's by a relative error of at most 0.015.
Values may be sent and summed in bfloat16 or wider, within the bound.
A program may use at most 128 MiB of HBM per device.

```python
import math
import jax
import jax.numpy as jnp
from jax import lax

D = 4096
SW = 2048
GROUP_CH = 16
STATE = 64
HEADS = 8
HD = 128
CHANNEL_GROUPS = 128
VD = 256
SEQUENCE_LENGTH = 512
SEQUENCE_COUNT = 4
N_TP = 2


def query_base(key):
    base = jax.random.normal(jax.random.fold_in(key, 101), (D, 2 * HEADS * HD), jnp.float32)
    return jnp.clip(base, -6.0, 6.0)


def draw_w_query(key, part):
    scale = 1.3 * D ** (-0.5)
    return (query_base(key) * scale).astype(jnp.bfloat16)


def draw_w_key(key, part):
    scale = 1.3 * D ** (-0.5)
    other = jnp.clip(jax.random.normal(jax.random.fold_in(key, 102), (D, 2 * HEADS * HD), jnp.float32), -6.0, 6.0)
    mixed = other * scale
    return jnp.clip(mixed, -20.0 * D ** (-0.5), 20.0 * D ** (-0.5)).astype(jnp.bfloat16)


def draw_decay_re(key, part):
    share = 0.5
    slow = jax.random.uniform(jax.random.fold_in(key, 201), (CHANNEL_GROUPS, 1), jnp.float32) < share
    slow_rate = jnp.exp(jax.random.uniform(jax.random.fold_in(key, 202), (CHANNEL_GROUPS, STATE), jnp.float32, jnp.log(0.05), jnp.log(0.3))) / SEQUENCE_LENGTH
    fast_rate = jnp.exp(jax.random.uniform(jax.random.fold_in(key, 203), (CHANNEL_GROUPS, STATE), jnp.float32, jnp.log(1.0 / 100.0), jnp.log(1.0 / 30.0)))
    return -jnp.where(slow, slow_rate, fast_rate)


def draw_decay_shift(key, part):
    block_count = 16
    span = SEQUENCE_LENGTH // block_count
    rates = jnp.exp(jax.random.uniform(jax.random.fold_in(key, 301), (SEQUENCE_COUNT, CHANNEL_GROUPS, block_count), jnp.float32, jnp.log(0.3), jnp.log(3.0))) / SEQUENCE_LENGTH
    position_indices = jnp.arange(SEQUENCE_LENGTH, dtype=jnp.int32)
    block_index = jnp.minimum(position_indices // span, block_count - 1).astype(jnp.int32)
    spread_decay_rates = jnp.take(rates, block_index, axis=2)
    spike_position = jax.random.randint(jax.random.fold_in(key, 302), (SEQUENCE_COUNT, CHANNEL_GROUPS, 2), 0, SEQUENCE_LENGTH)
    spike_depth = jnp.log(jax.random.uniform(jax.random.fold_in(key, 303), (SEQUENCE_COUNT, CHANNEL_GROUPS, 2), jnp.float32, 0.6, 0.85))
    spike_hits = position_indices[None, None, None, :] == spike_position[..., None]
    spike_events = jnp.sum(jnp.where(spike_hits, spike_depth[..., None], 0.0), axis=2)
    return -spread_decay_rates + spike_events


def shard_levels(own_key, shape, pieces, least, largest):
    factor_of, own = 1.0, jax.random.fold_in(own_key, 6)
    for position, parts in pieces:
        heights = jnp.exp(jax.random.uniform(jax.random.fold_in(own, position), (parts,), jnp.float32, least / len(pieces), largest / len(pieces)))
        factor_of = factor_of * jnp.repeat(heights, shape[position] // parts).reshape([-1 if axis == position else 1 for axis in range(len(shape))])
    return factor_of


def normal_values(key, dims, scale, reach, shards=(), kind=jnp.bfloat16):
    drawn = jax.random.normal(key, dims, jnp.float32) * scale
    if len(shards) > 0:
        drawn = shard_levels(key, dims, shards, -0.22, 0.18) * drawn
    return jnp.clip(drawn, min=-reach, max=reach).astype(kind)


def setup_inputs(seed: int = 0) -> dict:
    seeds = jax.random.split(jax.random.key(seed), 20)
    return {
        "tokens": normal_values(seeds[0], (SEQUENCE_COUNT, SEQUENCE_LENGTH, D), 1.0, 6.0, ((0, 4), (1, 4), (2, 2))),
        "norm_gain": jnp.clip(1.0 + 0.18 * jax.random.normal(seeds[1], (D,), jnp.float32), 0.1, 1.9),
        "w_state_in": normal_values(seeds[2], (D, SW), D ** -0.5, 0.09375, ((0, 16), (1, 2))),
        "w_query": draw_w_query(jax.random.fold_in(seeds[19], 71), 0),
        "w_key": draw_w_key(jax.random.fold_in(seeds[19], 71), 0),
        "w_value": normal_values(seeds[5], (D, HEADS * VD), D ** -0.5, 0.09375, ((0, 16), (1, 2))),
        "decay_re": draw_decay_re(jax.random.fold_in(seeds[19], 71), 0),
        "decay_im": jnp.clip(jax.random.uniform(seeds[7], (CHANNEL_GROUPS, STATE), jnp.float32, -3.140625, 3.140625), -3.140625, 3.140625),
        "log_step": jnp.clip(-3.5 + 2.0 * jax.random.uniform(seeds[8], (CHANNEL_GROUPS,), jnp.float32) ** shard_levels(seeds[8], (CHANNEL_GROUPS,), ((0, 2),), -0.2, 0.2), -3.5, -1.5),
        "decay_shift": draw_decay_shift(jax.random.fold_in(seeds[19], 71), 0),
        "in_re": normal_values(seeds[10], (CHANNEL_GROUPS, STATE, GROUP_CH), ((0.25 / GROUP_CH) ** 0.5), 2.0, ((0, 2),), jnp.float32),
        "in_im": normal_values(seeds[11], (CHANNEL_GROUPS, STATE, GROUP_CH), ((0.25 / GROUP_CH) ** 0.5), 2.0, ((0, 2),), jnp.float32),
        "output_real": normal_values(seeds[12], (CHANNEL_GROUPS, GROUP_CH, STATE), STATE ** -0.5, 0.75, ((0, 2),), jnp.float32),
        "output_imaginary": normal_values(seeds[13], (CHANNEL_GROUPS, GROUP_CH, STATE), STATE ** -0.5, 0.75, ((0, 2),), jnp.float32),
        "skip": normal_values(seeds[14], (SW,), 0.3, 1.2, ((0, 2),), jnp.float32),
        "mix_weight": jnp.clip(0.3 + 0.5 * jax.random.uniform(seeds[15], (HEADS,), jnp.float32) ** shard_levels(seeds[15], (HEADS,), ((0, 2),), -0.2, 0.2), 0.3, 0.8),
        "head_gain": jnp.clip(1.0 + 0.18 * jax.random.normal(seeds[16], (VD,), jnp.float32), 0.1, 1.9),
        "w_out_state": normal_values(seeds[17], (SW, D), SW ** -0.5, 0.125, ((0, 2),)),
        "w_out_attn": normal_values(seeds[18], (HEADS * VD, D), (HEADS * VD) ** -0.5, 0.125, ((0, 2),)),
    }


def compose(earlier, later):
    early_scale_re, early_scale_im, early_shift_re, early_shift_im = earlier
    late_scale_re, late_scale_im, late_shift_re, late_shift_im = later
    scale_re = late_scale_re * early_scale_re - late_scale_im * early_scale_im
    scale_im = late_scale_re * early_scale_im + late_scale_im * early_scale_re
    shift_re = late_scale_re * early_shift_re - late_scale_im * early_shift_im + late_shift_re
    shift_im = late_scale_re * early_shift_im + late_scale_im * early_shift_re + late_shift_im
    return (scale_re, scale_im, shift_re, shift_im)

def input_matrices(decay_re, decay_im, log_step, in_re, in_im):
    step_size = jnp.exp(log_step)[:, None]
    numer_re = jnp.expm1(decay_re) * jnp.cos(decay_im) - 2.0 * jnp.sin(0.5 * decay_im) ** 2
    numer_im = jnp.exp(decay_re) * jnp.sin(decay_im)
    modulus = decay_re * decay_re + decay_im * decay_im
    coef_re = step_size * (numer_re * decay_re + numer_im * decay_im) / modulus
    coef_im = step_size * (numer_im * decay_re - numer_re * decay_im) / modulus
    matrix_re = coef_re[..., None] * in_re - coef_im[..., None] * in_im
    matrix_im = coef_re[..., None] * in_im + coef_im[..., None] * in_re
    return (matrix_re, matrix_im)

def reference(tokens, norm_gain, w_state_in, w_query, w_key, w_value, decay_re, decay_im, log_step, decay_shift, in_re, in_im, output_real, output_imaginary, skip, mix_weight, head_gain, w_out_state, w_out_attn):
    upper_limit = lax.Precision.HIGHEST
    seq_count, seq_len, width = tokens.shape
    floats = tokens.astype(jnp.float32)
    normed = (floats * lax.rsqrt(lax.optimization_barrier(jnp.mean(floats * floats, axis=-1, keepdims=True)) + 1e-06) * norm_gain).astype(jnp.bfloat16)
    flat = normed.reshape(seq_count * seq_len, width)
    state_in = jnp.dot(flat, w_state_in, preferred_element_type=jnp.float32).astype(jnp.bfloat16)
    queries = jnp.dot(flat, w_query, preferred_element_type=jnp.float32).astype(jnp.bfloat16)
    keys = jnp.dot(flat, w_key, preferred_element_type=jnp.float32).astype(jnp.bfloat16)
    values = jnp.dot(flat, w_value, preferred_element_type=jnp.float32).astype(jnp.bfloat16)
    matrix_re, matrix_im = input_matrices(decay_re, decay_im, log_step, in_re, in_im)
    grouped = state_in.astype(jnp.float32).reshape(seq_count, seq_len, CHANNEL_GROUPS, GROUP_CH).transpose(2, 0, 1, 3)
    skip_grouped = skip.reshape(CHANNEL_GROUPS, GROUP_CH)

    def one_group(items):
        inputs, mat_re, mat_im, rate_re, rate_im, shift, read_re, read_im, direct = items
        drive_re = jnp.einsum('pc,slc->slp', mat_re, inputs, precision=upper_limit)
        drive_im = jnp.einsum('pc,slc->slp', mat_im, inputs, precision=upper_limit)
        magnitude = jnp.exp(rate_re[None, None, :] + shift[:, :, None])
        factor_re = magnitude * jnp.cos(rate_im)[None, None, :]
        factor_im = magnitude * jnp.sin(rate_im)[None, None, :]
        scanned = lax.associative_scan(compose, (factor_re, factor_im, drive_re, drive_im), axis=1)
        result = jnp.einsum('cp,slp->slc', read_re, scanned[2], precision=upper_limit) - jnp.einsum('cp,slp->slc', read_im, scanned[3], precision=upper_limit) + direct[None, None, :] * inputs
        return result
    group_out = lax.map(one_group, (grouped, matrix_re, matrix_im, decay_re, decay_im, decay_shift.transpose(1, 0, 2), output_real, output_imaginary, skip_grouped))
    state_out = group_out.transpose(1, 2, 0, 3).reshape(seq_count * seq_len, SW).astype(jnp.bfloat16)
    head_queries = queries.reshape(seq_count, seq_len, HEADS, 2, HD).transpose(0, 2, 1, 3, 4).reshape(seq_count * HEADS, seq_len, 2, HD)
    head_keys = keys.reshape(seq_count, seq_len, HEADS, 2, HD).transpose(0, 2, 1, 3, 4).reshape(seq_count * HEADS, seq_len, 2, HD)
    head_values = values.reshape(seq_count, seq_len, HEADS, VD).transpose(0, 2, 1, 3).reshape(seq_count * HEADS, seq_len, VD)
    head_mix = jnp.tile(mix_weight, seq_count)
    block = math.gcd(seq_len, 512)
    key_pos = jnp.arange(seq_len, dtype=jnp.int32)

    def one_head(items):
        query_all, key_all, value_all, lam = items
        key_float = key_all.astype(jnp.float32)
        value_float = value_all.astype(jnp.float32)

        def one_block(index):
            start = index * block
            query_block = lax.dynamic_slice_in_dim(query_all, start, block, 0).astype(jnp.float32)
            scores = jnp.einsum('qmd,kmd->mqk', query_block, key_float, precision=upper_limit) * HD ** (-0.5)
            query_pos = start + jnp.arange(block, dtype=jnp.int32)
            allowed = key_pos[None, :] <= query_pos[:, None]
            masked = jnp.where(allowed[None], scores, -1e+30)
            row_max = lax.optimization_barrier(jnp.max(masked, axis=-1))
            weights = jnp.where(allowed[None], jnp.exp(masked - row_max[..., None]), 0.0)
            total = lax.optimization_barrier(jnp.sum(weights, axis=-1))
            rounded = lax.optimization_barrier(weights.astype(jnp.bfloat16)).astype(jnp.float32)
            numer = jnp.einsum('mqk,kd->mqd', rounded, value_float, precision=upper_limit)
            head_raw = numer[0] / total[0][:, None] - lam * numer[1] / total[1][:, None]
            normed_head = head_raw * lax.rsqrt(lax.optimization_barrier(jnp.mean(head_raw * head_raw, axis=-1, keepdims=True)) + 1e-05) * head_gain
            return (normed_head.astype(jnp.bfloat16), row_max + jnp.log(total))
        outs, logs = lax.map(one_block, jnp.arange(seq_len // block, dtype=jnp.int32))
        return (outs.reshape(seq_len, VD), logs.transpose(1, 0, 2).reshape(2, seq_len))
    head_out, head_logs = lax.map(one_head, (head_queries, head_keys, head_values, head_mix))
    attn_out = head_out.reshape(seq_count, HEADS, seq_len, VD).transpose(0, 2, 1, 3).reshape(seq_count * seq_len, HEADS * VD)
    log_totals = head_logs.reshape(seq_count, HEADS, 2, seq_len)
    state_parts = state_out.reshape(seq_count * seq_len, N_TP, SW // N_TP)
    attn_parts = attn_out.reshape(seq_count * seq_len, N_TP, HEADS * VD // N_TP)
    state_weights = w_out_state.reshape(N_TP, SW // N_TP, width)
    attn_weights = w_out_attn.reshape(N_TP, HEADS * VD // N_TP, width)

    def add_part(total, index):
        term = jnp.dot(state_parts[:, index], state_weights[index], preferred_element_type=jnp.float32) + jnp.dot(attn_parts[:, index], attn_weights[index], preferred_element_type=jnp.float32)
        rounded = lax.optimization_barrier(term.astype(jnp.bfloat16)).astype(jnp.float32)
        return (total + rounded, None)
    summed, _ = lax.scan(add_part, jnp.zeros((seq_count * seq_len, width), jnp.float32), jnp.arange(N_TP, dtype=jnp.int32))
    mixed = summed.astype(jnp.bfloat16).reshape(seq_count, seq_len, width)
    return (mixed, log_totals)
```

```python
import functools
import math

import jax
import jax.numpy as jnp
from jax import lax
from jax.experimental import pallas as pl
from jax.experimental.pallas import tpu as pltpu
from jax.sharding import PartitionSpec as P


def prefix(x, axis, combine, identity):
    size, here = (lax.axis_size(axis), lax.axis_index(axis))
    everything = jax.tree.map(lambda part: lax.all_gather(part, axis), x)
    start = jax.tree.map(
        lambda part, zero: jnp.broadcast_to(jnp.asarray(zero, part.dtype), part.shape), x, identity
    )

    def hop(k, before):
        reached = k < here
        new = combine(before, jax.tree.map(lambda part: part[k], everything))
        return jax.tree.map(lambda a, b: jnp.where(reached, a, b), new, before)

    return lax.fori_loop(0, size, hop, start)


def compose(earlier, later):
    early_scale_re, early_scale_im, early_shift_re, early_shift_im = earlier
    late_scale_re, late_scale_im, late_shift_re, late_shift_im = later
    scale_re = late_scale_re * early_scale_re - late_scale_im * early_scale_im
    scale_im = late_scale_re * early_scale_im + late_scale_im * early_scale_re
    shift_re = late_scale_re * early_shift_re - late_scale_im * early_shift_im + late_shift_re
    shift_im = late_scale_re * early_shift_im + late_scale_im * early_shift_re + late_shift_im
    return (scale_re, scale_im, shift_re, shift_im)


def state_branch(
    state_in,
    decay_re,
    decay_im,
    log_step,
    decay_shift,
    in_re,
    in_im,
    output_real,
    output_imaginary,
    skip,
):
    upper_limit = lax.Precision.HIGHEST
    tok_rows = state_in.shape[0]
    group_count, state_size = decay_re.shape
    group_width = in_re.shape[2]
    flat_width = group_count * state_size
    step_size = jnp.exp(log_step)[:, None]
    numer_re = jnp.expm1(decay_re) * jnp.cos(decay_im) - 2.0 * jnp.sin(0.5 * decay_im) ** 2
    numer_im = jnp.exp(decay_re) * jnp.sin(decay_im)
    modulus = decay_re * decay_re + decay_im * decay_im
    coef_re = step_size * (numer_re * decay_re + numer_im * decay_im) / modulus
    coef_im = step_size * (numer_im * decay_re - numer_re * decay_im) / modulus
    matrix_re = coef_re[..., None] * in_re - coef_im[..., None] * in_im
    matrix_im = coef_re[..., None] * in_im + coef_im[..., None] * in_re
    inputs = state_in.astype(jnp.float32).reshape(tok_rows, group_count, group_width)
    flat_shape = (tok_rows, flat_width)
    drive_re = jnp.einsum("gpc,tgc->tgp", matrix_re, inputs, precision=upper_limit).reshape(
        flat_shape
    )
    drive_im = jnp.einsum("gpc,tgc->tgp", matrix_im, inputs, precision=upper_limit).reshape(
        flat_shape
    )
    magnitude = jnp.exp(decay_re[None] + decay_shift[0].T[:, :, None])
    factor_re = (magnitude * jnp.cos(decay_im)[None]).reshape(flat_shape)
    factor_im = (magnitude * jnp.sin(decay_im)[None]).reshape(flat_shape)
    span = math.gcd(tok_rows, 16)
    block_count = tok_rows // span

    def to_blocks(values):
        return values.reshape(block_count, span, flat_width).transpose(1, 0, 2)

    rows_in = tuple((to_blocks(values) for values in (factor_re, factor_im, drive_re, drive_im)))
    ones_blocks = jnp.ones((block_count, flat_width), jnp.float32)
    zero_blocks = jnp.zeros((block_count, flat_width), jnp.float32)

    def row_step(carry, row):
        joined = compose(carry, row)
        return (joined, joined)

    block_totals, local = lax.scan(
        row_step, (ones_blocks, zero_blocks, zero_blocks, zero_blocks), rows_in
    )
    ones_row = jnp.ones((flat_width,), jnp.float32)
    zero_row = jnp.zeros((flat_width,), jnp.float32)

    def block_step(carry, row):
        return (compose(carry, row), carry)

    totals, before = lax.scan(block_step, (ones_row, zero_row, zero_row, zero_row), block_totals)
    carried = prefix(totals, "sp", compose, (ones_row, zero_row, zero_row, zero_row))
    start_re, start_im = (carried[2], carried[3])
    enter_re = before[0] * start_re[None] - before[1] * start_im[None] + before[2]
    enter_im = before[0] * start_im[None] + before[1] * start_re[None] + before[3]
    state_real = local[2] + local[0] * enter_re[None] - local[1] * enter_im[None]
    state_imaginary = local[3] + local[0] * enter_im[None] + local[1] * enter_re[None]
    group_layout_shape = (tok_rows, group_count, state_size)
    state_real = state_real.transpose(1, 0, 2).reshape(group_layout_shape)
    state_imaginary = state_imaginary.transpose(1, 0, 2).reshape(group_layout_shape)
    result = (
        jnp.einsum("hsv,jhv->jhs", output_real, state_real, precision=upper_limit)
        - jnp.einsum("hsv,jhv->jhs", output_imaginary, state_imaginary, precision=upper_limit)
        + skip.reshape(group_count, group_width)[None] * inputs
    )
    return result.reshape(tok_rows, group_count * group_width).astype(jnp.bfloat16)


def attention_branch(queries, keys_local, values_local, mix_weight, head_gain):
    tok_rows = queries.shape[0]
    head_count = mix_weight.shape[0]
    head_dim = queries.shape[1] // (2 * head_count)
    value_dim = values_local.shape[1] // head_count
    scale = head_dim ** (-0.5)
    first_pos = lax.axis_index("sp") * tok_rows
    query_pos = first_pos + jnp.arange(tok_rows, dtype=jnp.int32)
    query_heads = queries.reshape(tok_rows, head_count, 2, head_dim)
    initial = (
        jnp.full((head_count, 2, tok_rows), -1e30, jnp.float32),
        jnp.zeros((head_count, 2, tok_rows), jnp.float32),
        jnp.zeros((head_count, 2, tok_rows, value_dim), jnp.float32),
    )
    key_piece = lax.all_gather(keys_local, "sp", axis=0, tiled=True)
    value_piece = lax.all_gather(values_local, "sp", axis=0, tiled=True)
    count = key_piece.shape[0]
    block = math.gcd(count, 512)

    def one_block(index, inner):
        run_max, run_total, run_accum = inner
        offset = index * block
        key_block = lax.dynamic_slice_in_dim(key_piece, offset, block, 0).reshape(
            block, head_count, 2, head_dim
        )
        value_block = lax.dynamic_slice_in_dim(value_piece, offset, block, 0).reshape(
            block, head_count, value_dim
        )
        key_pos = offset + jnp.arange(block, dtype=jnp.int32)
        scores = (
            jnp.einsum(
                "qhmd,khmd->hmqk", query_heads, key_block, preferred_element_type=jnp.float32
            )
            * scale
        )
        allowed = key_pos[None, :] <= query_pos[:, None]
        masked = jnp.where(allowed, scores, -1e30)
        new_max = jnp.maximum(run_max, jnp.max(masked, axis=-1))
        weights = jnp.where(allowed, jnp.exp(masked - new_max[..., None]), 0.0)
        rescale = jnp.exp(run_max - new_max)
        new_total = run_total * rescale + jnp.sum(weights, axis=-1)
        product = jnp.einsum(
            "hmqk,khd->hmqd",
            weights.astype(jnp.bfloat16),
            value_block,
            preferred_element_type=jnp.float32,
        )
        return (new_max, new_total, run_accum * rescale[..., None] + product)

    def visit(inner):
        return lax.fori_loop(0, count // block, one_block, inner)

    def keep_carry(inner):
        return inner

    maxima, totals, accum = lax.cond(
        jnp.int32(0) <= first_pos + tok_rows - 1, visit, keep_carry, initial
    )
    log_totals = maxima + jnp.log(totals)
    head_raw = (
        accum[:, 0] / totals[:, 0, :, None]
        - mix_weight[:, None, None] * accum[:, 1] / totals[:, 1, :, None]
    )
    normed_heads = (
        head_raw
        * lax.rsqrt(jnp.mean(head_raw * head_raw, axis=-1, keepdims=True) + 1e-05)
        * head_gain
    )
    attn_out = (
        normed_heads.transpose(1, 0, 2)
        .reshape(tok_rows, head_count * value_dim)
        .astype(jnp.bfloat16)
    )
    return (attn_out, log_totals)


def per_device(
    tokens,
    norm_gain,
    w_state_in,
    w_query,
    w_key,
    w_value,
    decay_re,
    decay_im,
    log_step,
    decay_shift,
    in_re,
    in_im,
    output_real,
    output_imaginary,
    skip,
    mix_weight,
    head_gain,
    w_out_state,
    w_out_attn,
):
    whole = lax.all_gather(tokens, "tp", axis=2, tiled=True)[0]
    floats = whole.astype(jnp.float32)
    normed = (
        floats * lax.rsqrt(jnp.mean(floats * floats, axis=-1, keepdims=True) + 1e-06) * norm_gain
    ).astype(jnp.bfloat16)
    pieces = (
        lax.all_gather(w_state_in, ("sp", "fs"), axis=0, tiled=True),
        lax.all_gather(w_query, ("sp", "fs"), axis=0, tiled=True),
        lax.all_gather(w_key, ("sp", "fs"), axis=0, tiled=True),
        lax.all_gather(w_value, ("sp", "fs"), axis=0, tiled=True),
    )
    sums = tuple((jnp.dot(normed, piece, preferred_element_type=jnp.float32) for piece in pieces))
    state_in = sums[0].astype(jnp.bfloat16)
    queries = sums[1].astype(jnp.bfloat16)
    keys_local = sums[2].astype(jnp.bfloat16)
    values_local = sums[3].astype(jnp.bfloat16)
    attn_out, log_totals = attention_branch(
        queries, keys_local, values_local, mix_weight, head_gain
    )
    state_out = state_branch(
        state_in,
        decay_re,
        decay_im,
        log_step,
        decay_shift,
        in_re,
        in_im,
        output_real,
        output_imaginary,
        skip,
    )
    summed = lax.psum_scatter(
        (
            jnp.dot(state_out, w_out_state, preferred_element_type=jnp.float32)
            + jnp.dot(attn_out, w_out_attn, preferred_element_type=jnp.float32)
        ).astype(jnp.bfloat16),
        "tp",
        scatter_dimension=0,
        tiled=True,
    )
    return (summed[None], log_totals[None])


def nt_dot(a, b):
    return lax.dot_general(a, b, (((1,), (1,)), ((), ())), preferred_element_type=jnp.float32)


def split_pair(x):
    high = x.astype(jnp.bfloat16)
    low = (x - high.astype(jnp.float32)).astype(jnp.bfloat16)
    return (high, low)


def small_expm1(x):
    total = jnp.ones_like(x)
    for n in range(9, 1, -1):
        total = 1.0 + total * x * (1.0 / n)
    return total * x


def fused_kernel(
    sizes,
    tok_ref,
    gain_ref,
    ws_ref,
    wq_ref,
    wk_ref,
    wv_ref,
    dre_ref,
    dim_ref,
    logstep_ref,
    shift_ref,
    inre_ref,
    inim_ref,
    outre_ref,
    outim_ref,
    skip_ref,
    mix_ref,
    hgain_ref,
    wos_ref,
    woa_ref,
    mixed_ref,
    logt_ref,
    stat_send,
    stat_recv,
    nbuf,
    xbuf,
    wbuf,
    pbuf,
    rbuf,
    fin,
    shsend,
    shbuf,
    inbuf,
    outbuf,
    coef,
    etab,
    bcat,
    ccat,
    srow,
    yacc,
    stb,
    atb,
    sto,
    ato,
    ltb,
    lto,
    wo,
    acc,
    poutb,
    precb,
    loc_sem,
    wo_sem,
    w_loc,
    stat_sem,
    tok_send,
    tok_recv,
    fwd_send,
    wx_send,
    wx_recv,
    wy_send,
    wy_recv,
    dx_send,
    dx_recv,
    dy_send,
    dy_recv,
    z_send,
    z_recv,
    sh_send,
    sh_recv,
    st_send,
    st_recv,
    at_send,
    at_recv,
    lt_send,
    lt_recv,
    p_send,
    p_recv,
):
    NS, NT, L, D, CW = sizes
    KW = D // NS
    FW = D // NT
    NB = NS // NT
    HC = CW // NS
    SEQ = NS * L
    G = HC // 16
    MESH = pl.DeviceIdType.MESH
    s, f, c = (lax.axis_index("sp"), lax.axis_index("fs"), lax.axis_index("tp"))
    fx = f + 1 - 2 * lax.rem(f, 2)
    fy = lax.rem(f + 2, 4)
    fd = 3 - f
    partner = {"tp": 1 - c}
    owner = s // NB

    def remote(src, dst, send, recv, where):
        return pltpu.make_async_remote_copy(
            src_ref=src, dst_ref=dst, send_sem=send, recv_sem=recv, device_id=where, device_id_type=MESH
        )

    g0 = pl.multiple_of(s * G, G)
    own_w = [
        pltpu.make_async_copy(ref, wbuf.at[m, f], w_loc.at[m])
        for m, ref in enumerate((ws_ref, wq_ref, wk_ref, wv_ref))
    ]
    for copy in own_w:
        copy.start()
    own_p = [
        pltpu.make_async_copy(ref.at[pl.ds(g0, G)], dst, loc_sem.at[i])
        for i, (ref, dst) in enumerate(
            (
                (inre_ref, inbuf.at[0]),
                (inim_ref, inbuf.at[1]),
                (outre_ref, outbuf.at[0]),
                (outim_ref, outbuf.at[1]),
            )
        )
    ]
    for copy in own_p:
        copy.start()
    big = [pltpu.make_async_copy(ref, wo.at[i], wo_sem.at[i]) for i, ref in enumerate((wos_ref, woa_ref))]
    for copy in big:
        copy.start()

    barrier = pltpu.get_barrier_semaphore()
    pl.semaphore_signal(barrier, inc=1, device_id={"fs": fx}, device_id_type=MESH)
    pl.semaphore_signal(barrier, inc=1, device_id={"fs": fy}, device_id_type=MESH)
    pl.semaphore_signal(barrier, inc=1, device_id=partner, device_id_type=MESH)
    for k in range(1, NS):
        pl.semaphore_signal(barrier, inc=1, device_id={"sp": lax.rem(s + k, NS)}, device_id_type=MESH)
    pl.semaphore_wait(barrier, 2 + NS)

    def own_x(m):
        return remote(wbuf.at[m, f], wbuf.at[m, f], wx_send.at[m], wx_recv.at[m], {"fs": fx})

    def own_y(m):
        return remote(wbuf.at[m, f], wbuf.at[m, f], wy_send.at[m], wy_recv.at[m], {"fs": fy})

    half = wbuf.shape[2] // 2

    def fwd_y(m):
        part = wbuf.at[m, fx, pl.ds(0, half)]
        return remote(part, part, dy_send.at[m], dy_recv.at[m], {"fs": fy})

    def fwd_x(m):
        part = wbuf.at[m, fy, pl.ds(half, half)]
        return remote(part, part, dx_send.at[m], dx_recv.at[m], {"fs": fx})

    tokens = tok_ref[0].astype(jnp.float32)
    square = jnp.sum(tokens * tokens, axis=1, keepdims=True)
    stat_send[...] = jnp.broadcast_to(square, (L, 128))
    stat = remote(stat_send, stat_recv, stat_sem.at[0], stat_sem.at[1], partner)
    stat.start()
    for m in range(4):
        own_w[m].wait()
    for m in range(2):
        own_x(m).start()
        own_y(m).start()
    for d in range(NS):
        shsend[d] = shift_ref[0, d * G : (d + 1) * G, :]
    for k in range(1, NS):
        d = lax.rem(s + k, NS)
        remote(shsend.at[d], shbuf.at[s], sh_send.at[d], sh_recv.at[s], {"sp": d}).start()
    shbuf[s] = shsend[s]
    stat.wait()
    mean = (square + stat_recv[:, 0:1]) * (1.0 / D)
    gain = gain_ref[:, pl.ds(pl.multiple_of(c * FW, FW), FW)]
    normed = (tok_ref[0].astype(jnp.float32) * lax.rsqrt(mean + 1e-06) * gain).astype(jnp.bfloat16)

    def tok_copy(i):
        return remote(
            nbuf.at[i], xbuf.at[s], tok_send.at[i], tok_recv.at[s], {"sp": c * NB + i}
        )

    for i in range(NB):
        nbuf[i] = normed[:, i * KW : (i + 1) * KW]
    for i in range(NB):
        @pl.when(c * NB + i != s)
        def _():
            tok_copy(i).start()

        @pl.when(c * NB + i == s)
        def _():
            xbuf[s] = nbuf[i]

    def tok_forward(q):
        return remote(xbuf.at[q], xbuf.at[q], fwd_send.at[q], tok_recv.at[q], partner)

    def tok_arrival(q):
        return remote(xbuf.at[q], xbuf.at[q], fwd_send.at[q], tok_recv.at[q], partner)

    re16 = dre_ref[pl.ds(g0, G), :]
    im16 = dim_ref[pl.ds(g0, G), :]
    re16 = jnp.concatenate([re16, re16], axis=1)
    im16 = jnp.concatenate([im16, im16], axis=1)
    numer_re = small_expm1(re16) * jnp.cos(im16) - 2.0 * jnp.sin(0.5 * im16) ** 2
    numer_im = jnp.exp(re16) * jnp.sin(im16)
    modulus = re16 * re16 + im16 * im16
    coef[0] = re16
    coef[1] = im16
    coef[2] = (numer_re * re16 + numer_im * im16) / modulus
    coef[3] = (numer_im * re16 - numer_re * im16) / modulus
    for copy in own_p:
        copy.wait()
    lane = lax.broadcasted_iota(jnp.int32, (128, 16), 0)
    chan = lax.broadcasted_iota(jnp.int32, (128, 16), 1)
    steps = lax.broadcasted_iota(jnp.int32, (L, 128), 0).astype(jnp.float32) + 1.0
    sel_hi = lax.broadcasted_iota(jnp.int32, (128, 16), 0)

    def table(g, carry):
        zr = coef[0, pl.ds(g, 1), :]
        zi = coef[1, pl.ds(g, 1), :]
        step = jnp.exp(jnp.full((1, 128), logstep_ref[g0 + g], jnp.float32))
        cr = coef[2, pl.ds(g, 1), :] * step
        ci = coef[3, pl.ds(g, 1), :] * step
        angle = steps * zi
        cosine, sine = (jnp.cos(angle), jnp.sin(angle))
        shrink = jnp.exp(steps * zr)
        grow = jnp.exp(-(steps * zr))
        etab[0, g] = grow * (cosine * cr + sine * ci)
        etab[1, g] = grow * (cosine * ci - sine * cr)
        etab[2, g] = shrink * cosine
        etab[3, g] = shrink * sine
        pick = (lane == lax.rem(g, 8) * 16 + chan).astype(jnp.bfloat16)
        ir, ii = (inbuf[0, g], inbuf[1, g])
        raw = jnp.concatenate([ir, ii, -ii, ir], axis=0)
        hi, lo = split_pair(raw)
        bcat[g] = jnp.concatenate(
            [nt_dot(hi, pick).astype(jnp.bfloat16), nt_dot(lo, pick).astype(jnp.bfloat16)], axis=1
        )
        cr_, ci_ = (outbuf[0, g], outbuf[1, g])
        rawc = jnp.concatenate([cr_, -ci_, -ci_, -cr_], axis=1)
        hi, lo = split_pair(rawc)
        ccat[g] = jnp.concatenate(
            [
                jnp.dot(pick, hi, preferred_element_type=jnp.float32).astype(jnp.bfloat16),
                jnp.dot(pick, lo, preferred_element_type=jnp.float32).astype(jnp.bfloat16),
            ],
            axis=0,
        )
        return carry

    lax.fori_loop(0, G, table, 0)
    for k in range(1, NS):
        q = lax.rem(s + k, NS)
        remote(shsend.at[q], shbuf.at[q], sh_send.at[q], sh_recv.at[q], {"sp": q}).wait_recv()
    row_i = lax.broadcasted_iota(jnp.int32, (L, L), 0)
    col_i = lax.broadcasted_iota(jnp.int32, (L, L), 1)
    upper = (row_i <= col_i).astype(jnp.float32)
    for k in range(NS):
        srow[k] = jnp.dot(
            shbuf[k], upper, precision=lax.Precision.HIGHEST, preferred_element_type=jnp.float32
        )

    for k in range(NS):
        q = lax.rem(s + k, NS)

        @pl.when(c == owner)
        def _():
            @pl.when(q != s)
            def _():
                tok_arrival(q).wait_recv()

            tok_forward(q).start()

        @pl.when(c != owner)
        def _():
            tok_arrival(q).wait_recv()

    def z_copy(m, d):
        return remote(pbuf.at[m, d], rbuf.at[m, s], z_send.at[m, d], z_recv.at[m, s], {"sp": d})

    def project(m, carry):
        own_x(m).wait_recv()
        own_y(m).wait_recv()
        fwd_y(m).start()
        fwd_x(m).start()

        @pl.when(m < 2)
        def _():
            own_x(m + 2).start()
            own_y(m + 2).start()

        diag_y = wbuf.at[m, fd, pl.ds(0, half)]
        diag_x = wbuf.at[m, fd, pl.ds(half, half)]
        remote(diag_y, diag_y, dy_send.at[m], dy_recv.at[m], {"fs": fy}).wait_recv()
        remote(diag_x, diag_x, dx_send.at[m], dx_recv.at[m], {"fs": fx}).wait_recv()

        def block(k, inner):
            d = lax.rem(s + k + 1, NS)
            columns = pl.ds(pl.multiple_of(d * HC, HC), HC)
            lhs = xbuf[...].reshape(SEQ, KW)
            rhs = wbuf[m, :, :, columns].reshape(KW, HC)
            part = jnp.dot(lhs, rhs, preferred_element_type=jnp.float32).astype(jnp.bfloat16)

            @pl.when(k < NS - 1)
            def _():
                pbuf[m, d] = part
                z_copy(m, d).start()

            @pl.when(k == NS - 1)
            def _():
                rbuf[m, s] = part

            return inner

        return lax.fori_loop(0, NS, block, carry)

    def finish(m):
        for k in range(1, NS):
            q = lax.rem(s + k, NS)
            remote(pbuf.at[m, q], rbuf.at[m, q], z_send.at[m, q], z_recv.at[m, q], {"sp": q}).wait_recv()
        total = rbuf[m, 0].astype(jnp.float32)
        for q in range(1, NS):
            total = total + rbuf[m, q].astype(jnp.float32)
        fin[m] = total.astype(jnp.bfloat16)

    lax.fori_loop(0, 2, project, 0)

    finish(0)
    sign = jnp.where(lax.broadcasted_iota(jnp.int32, (8, 128), 1) < 64, -1.0, 1.0)
    lower = row_i >= col_i

    def lane_block(b, carry):
        lanes = pl.ds(pl.multiple_of(b * 128, 128), 128)
        u = fin[0, :, lanes]
        uu = jnp.concatenate([u, u], axis=1)
        yacc[...] = jnp.zeros_like(yacc)

        def group(g8, inner):
            g = b * 8 + g8
            drives = nt_dot(uu, bcat[g])
            h = jnp.zeros((1, 128), jnp.float32)
            er, ei, fr, fi = (etab[0, g], etab[1, g], etab[2, g], etab[3, g])
            for k in range(NS):
                d = drives[k * L : (k + 1) * L]
                x = er * d[:, :128] + ei * d[:, 128:]
                xh, xl = split_pair(x)
                xx = jnp.concatenate([xh, xl], axis=1)
                rhs = jnp.concatenate([xx, xx], axis=0)
                sr = jnp.broadcast_to(srow[k, pl.ds(g, 1), :], (L, L))
                sc = sr.T
                mask = jnp.where(lower, jnp.exp(jnp.minimum(sc - sr, 0.0)), 0.0)
                mh, ml = split_pair(mask)
                w2 = jnp.dot(
                    jnp.concatenate([mh, ml], axis=1), rhs, preferred_element_type=jnp.float32
                )
                q = w2[:, :128] + w2[:, 128:] + jnp.exp(sc) * h
                p1 = q * fr
                p2 = q * fi
                tail = p1[L - 8 :] + sign * pltpu.roll(p2[L - 8 :], 64, 1)
                h = tail[7:8]
                ph, plow = split_pair(jnp.concatenate([p1, p2], axis=1))
                y2 = nt_dot(ph, ccat[g]) + nt_dot(plow, ccat[g])
                yacc[k * L : (k + 1) * L, :] += y2[:, :128] + y2[:, 128:]
            return inner

        lax.fori_loop(0, 8, group, 0)
        direct = skip_ref[:, pl.ds(pl.multiple_of(s * HC + b * 128, 128), 128)]
        out = (yacc[...] + direct * u.astype(jnp.float32)).astype(jnp.bfloat16)
        for k in range(NS):
            stb[k, :, lanes] = out[k * L : (k + 1) * L]
        return carry

    lax.fori_loop(0, HC // 128, lane_block, 0)

    lax.fori_loop(2, 4, project, 0)

    def st_copy(d):
        return remote(stb.at[d], sto.at[s], st_send.at[d], st_recv.at[s], {"sp": d})

    def at_copy(d):
        return remote(atb.at[d], ato.at[s], at_send.at[d], at_recv.at[s], {"sp": d})

    def lt_copy(d):
        return remote(ltb.at[d], lto.at[s], lt_send.at[d], lt_recv.at[s], {"sp": d})

    for k in range(1, NS):
        st_copy(lax.rem(s + k, NS)).start()
    sto[s] = stb[s]

    hd = HC // 2
    finish(1)
    finish(2)
    finish(3)
    lam = mix_ref[s]
    for i in range(NS):
        width = (i + 1) * L
        heads = []
        for m in range(2):
            sc = nt_dot(
                fin[1, i * L : (i + 1) * L, m * hd : (m + 1) * hd], fin[2, 0:width, m * hd : (m + 1) * hd]
            ) * (hd ** (-0.5))
            qpos = lax.broadcasted_iota(jnp.int32, (L, width), 0) + i * L
            kpos = lax.broadcasted_iota(jnp.int32, (L, width), 1)
            allowed = kpos <= qpos
            sc = jnp.where(allowed, sc, -1e30)
            top = jnp.max(sc, axis=1, keepdims=True)
            weights = jnp.where(allowed, jnp.exp(sc - top), 0.0)
            total = jnp.sum(weights, axis=1, keepdims=True)
            value = jnp.dot(
                weights.astype(jnp.bfloat16), fin[3, 0:width, :], preferred_element_type=jnp.float32
            )
            heads.append(value / total)
            logs = jnp.broadcast_to(top + jnp.log(total), (L, L)).T
            ltb[i, m : m + 1, :] = logs[0:1]
        raw = heads[0] - lam * heads[1]
        scale = lax.rsqrt(jnp.mean(raw * raw, axis=1, keepdims=True) + 1e-05)
        atb[i] = (raw * scale * hgain_ref[...]).astype(jnp.bfloat16)

    for k in range(1, NS):
        d = lax.rem(s + k, NS)
        at_copy(d).start()
        lt_copy(d).start()
    ato[s] = atb[s]
    lto[s] = ltb[s]

    for copy in big:
        copy.wait()
    for k in range(1, NS):
        q = lax.rem(s + k, NS)
        remote(stb.at[q], sto.at[q], st_send.at[q], st_recv.at[q], {"sp": q}).wait_recv()
    tiles = poutb.shape[0]
    width = D // tiles
    st_lhs = jnp.concatenate([sto[q] for q in range(NS)], axis=1)

    def state_tile(n, carry):
        columns = pl.ds(pl.multiple_of(n * width, width), width)
        acc[:, columns] = jnp.dot(st_lhs, wo[0, :, columns], preferred_element_type=jnp.float32)
        return carry

    lax.fori_loop(0, tiles, state_tile, 0)
    for k in range(1, NS):
        q = lax.rem(s + k, NS)
        remote(atb.at[q], ato.at[q], at_send.at[q], at_recv.at[q], {"sp": q}).wait_recv()
    at_lhs = jnp.concatenate([ato[q] for q in range(NS)], axis=1)
    rows = L // NT
    mine = pl.ds(pl.multiple_of(c * rows, rows), rows)

    def p_copy(n):
        theirs = pl.ds(pl.multiple_of((1 - c) * rows, rows), rows)
        return remote(poutb.at[n, theirs], precb.at[n], p_send.at[n], p_recv.at[n], partner)

    def attn_tile(n, carry):
        columns = pl.ds(pl.multiple_of(n * width, width), width)
        part = acc[:, columns] + jnp.dot(at_lhs, wo[1, :, columns], preferred_element_type=jnp.float32)
        poutb[n] = part.astype(jnp.bfloat16)
        p_copy(n).start()
        return carry

    lax.fori_loop(0, tiles, attn_tile, 0)

    def last_tile(n, carry):
        columns = pl.ds(pl.multiple_of(n * width, width), width)
        p_copy(n).wait()
        mixed_ref[0, :, columns] = (
            poutb[n, mine, :].astype(jnp.float32) + precb[n].astype(jnp.float32)
        ).astype(jnp.bfloat16)
        return carry

    lax.fori_loop(0, tiles, last_tile, 0)
    for k in range(1, NS):
        q = lax.rem(s + k, NS)
        remote(ltb.at[q], lto.at[q], lt_send.at[q], lt_recv.at[q], {"sp": q}).wait_recv()
    logt_ref[0] = lto[...]

    for m in range(4):
        own_x(m).wait_send()
        own_y(m).wait_send()
        fwd_x(m).wait_send()
        fwd_y(m).wait_send()
        for k in range(1, NS):
            z_copy(m, lax.rem(s + k, NS)).wait_send()
    for k in range(1, NS):
        d = lax.rem(s + k, NS)
        remote(shsend.at[d], shbuf.at[s], sh_send.at[d], sh_recv.at[s], {"sp": d}).wait_send()
        st_copy(d).wait_send()
        at_copy(d).wait_send()
        lt_copy(d).wait_send()
    for i in range(NB):
        @pl.when(c * NB + i != s)
        def _():
            tok_copy(i).wait_send()

    @pl.when(c == owner)
    def _():
        for q in range(NS):
            tok_forward(q).wait_send()


def fused_device(sizes, *args):
    (tokens, norm_gain, ws, wq, wk, wv, dre, dim, logstep, shift, inre, inim, outre, outim, skip, mix, hgain, wos, woa) = args
    NS, NT, L, D, CW = sizes
    KW, HC = (D // NS, CW // NS)
    SEQ, G, NB, NF = (NS * L, HC // 16, NS // NT, 4)
    tiles = 8
    bf, f32 = (jnp.bfloat16, jnp.float32)
    V = pltpu.VMEM
    DMA = pltpu.SemaphoreType.DMA
    vmem = pl.BlockSpec(memory_space=pltpu.VMEM)
    smem = pl.BlockSpec(memory_space=pltpu.SMEM)
    hbm = pl.BlockSpec(memory_space=pl.ANY)
    scratch = [
        V((L, 128), f32),
        V((L, 128), f32),
        V((NB, L, KW), bf),
        V((NS, L, KW), bf),
        V((4, NF, ws.shape[0], CW), bf),
        V((4, NS, SEQ, HC), bf),
        V((4, NS, SEQ, HC), bf),
        V((4, SEQ, HC), bf),
        V((NS, G, L), f32),
        V((NS, G, L), f32),
        V((2, G, 64, 16), f32),
        V((2, G, 16, 64), f32),
        V((4, G, 128), f32),
        V((4, G, L, 128), f32),
        V((G, 256, 256), bf),
        V((G, 256, 256), bf),
        V((NS, G, L), f32),
        V((SEQ, 128), f32),
        V((NS, L, HC), bf),
        V((NS, L, HC), bf),
        V((NS, L, HC), bf),
        V((NS, L, HC), bf),
        V((NS, 2, L), f32),
        V((NS, 2, L), f32),
        V((2, CW, D), bf),
        V((L, D), f32),
        V((tiles, L, D // tiles), bf),
        V((tiles, L // NT, D // tiles), bf),
        DMA((4,)),
        DMA((2,)),
        DMA((4,)),
        DMA((2,)),
        DMA((NB,)),
        DMA((NS,)),
        DMA((NS,)),
    ]
    scratch += [DMA((4,))] * 8
    scratch += [DMA((4, NS))] * 2
    scratch += [DMA((NS,))] * 8
    scratch += [DMA((tiles,))] * 2
    call = pl.pallas_call(
        functools.partial(fused_kernel, sizes),
        out_shape=(
            jax.ShapeDtypeStruct((1, L // NT, D), bf),
            jax.ShapeDtypeStruct((1, NS, 2, L), f32),
        ),
        in_specs=[vmem, vmem, hbm, hbm, hbm, hbm, vmem, vmem, smem, vmem, hbm, hbm, hbm, hbm, vmem, smem, vmem, hbm, hbm],
        out_specs=(vmem, vmem),
        scratch_shapes=scratch,
        compiler_params=pltpu.CompilerParams(
            collective_id=0, has_side_effects=True, vmem_limit_bytes=67043328
        ),
    )
    return call(
        tokens, norm_gain.reshape(1, -1), ws, wq, wk, wv, dre, dim, logstep, shift, inre, inim, outre, outim,
        skip.reshape(1, -1), mix, hgain.reshape(1, -1), wos, woa,
    )


def choose_device(sp, fs, tp, *args):
    tokens, ws, dre, inre, mix = (args[0], args[2], args[6], args[10], args[15])
    L, D = (tokens.shape[1], ws.shape[0] * sp * fs)
    CW = ws.shape[1]
    fits = (
        fs == 4
        and tp == 2
        and sp % tp == 0
        and mix.shape[0] == sp
        and L == 128
        and CW == sp * 256
        and dre.shape == (sp * 16, 64)
        and inre.shape[2] == 16
        and D % (sp * 128) == 0
    )
    if fits:
        return fused_device((sp, tp, L, D, CW), *args)
    return per_device(*args)


def solution(mesh):
    in_specs = (
        P("fs", "sp", "tp"),
        P(),
        P(("sp", "fs"), "tp"),
        P(("sp", "fs"), "tp"),
        P(("sp", "fs"), "tp"),
        P(("sp", "fs"), "tp"),
        P("tp", None),
        P("tp", None),
        P("tp"),
        P("fs", "tp", "sp"),
        P("tp", None, None),
        P("tp", None, None),
        P("tp", None, None),
        P("tp", None, None),
        P("tp"),
        P("tp"),
        P(),
        P("tp", None),
        P("tp", None),
    )
    out_specs = (P("fs", ("sp", "tp"), None), P("fs", "tp", None, "sp"))
    body = functools.partial(choose_device, mesh.shape["sp"], mesh.shape["fs"], mesh.shape["tp"])
    return jax.shard_map(
        body, mesh=mesh, in_specs=in_specs, out_specs=out_specs, check_vma=False
    )
```

```python
import functools
import math

import jax
import jax.numpy as jnp
from jax import lax
from jax.experimental import pallas as pl
from jax.experimental.pallas import tpu as pltpu
from jax.sharding import PartitionSpec as P


def prefix(x, axis, combine, identity):
    size, here = (lax.axis_size(axis), lax.axis_index(axis))
    everything = jax.tree.map(lambda part: lax.all_gather(part, axis), x)
    start = jax.tree.map(
        lambda part, zero: jnp.broadcast_to(jnp.asarray(zero, part.dtype), part.shape), x, identity
    )

    def hop(k, before):
        reached = k < here
        new = combine(before, jax.tree.map(lambda part: part[k], everything))
        return jax.tree.map(lambda a, b: jnp.where(reached, a, b), new, before)

    return lax.fori_loop(0, size, hop, start)


def compose(earlier, later):
    early_scale_re, early_scale_im, early_shift_re, early_shift_im = earlier
    late_scale_re, late_scale_im, late_shift_re, late_shift_im = later
    scale_re = late_scale_re * early_scale_re - late_scale_im * early_scale_im
    scale_im = late_scale_re * early_scale_im + late_scale_im * early_scale_re
    shift_re = late_scale_re * early_shift_re - late_scale_im * early_shift_im + late_shift_re
    shift_im = late_scale_re * early_shift_im + late_scale_im * early_shift_re + late_shift_im
    return (scale_re, scale_im, shift_re, shift_im)


def state_branch(
    state_in,
    decay_re,
    decay_im,
    log_step,
    decay_shift,
    in_re,
    in_im,
    output_real,
    output_imaginary,
    skip,
):
    upper_limit = lax.Precision.HIGHEST
    tok_rows = state_in.shape[0]
    group_count, state_size = decay_re.shape
    group_width = in_re.shape[2]
    flat_width = group_count * state_size
    step_size = jnp.exp(log_step)[:, None]
    numer_re = jnp.expm1(decay_re) * jnp.cos(decay_im) - 2.0 * jnp.sin(0.5 * decay_im) ** 2
    numer_im = jnp.exp(decay_re) * jnp.sin(decay_im)
    modulus = decay_re * decay_re + decay_im * decay_im
    coef_re = step_size * (numer_re * decay_re + numer_im * decay_im) / modulus
    coef_im = step_size * (numer_im * decay_re - numer_re * decay_im) / modulus
    matrix_re = coef_re[..., None] * in_re - coef_im[..., None] * in_im
    matrix_im = coef_re[..., None] * in_im + coef_im[..., None] * in_re
    inputs = state_in.astype(jnp.float32).reshape(tok_rows, group_count, group_width)
    flat_shape = (tok_rows, flat_width)
    drive_re = jnp.einsum("gpc,tgc->tgp", matrix_re, inputs, precision=upper_limit).reshape(
        flat_shape
    )
    drive_im = jnp.einsum("gpc,tgc->tgp", matrix_im, inputs, precision=upper_limit).reshape(
        flat_shape
    )
    magnitude = jnp.exp(decay_re[None] + decay_shift[0].T[:, :, None])
    factor_re = (magnitude * jnp.cos(decay_im)[None]).reshape(flat_shape)
    factor_im = (magnitude * jnp.sin(decay_im)[None]).reshape(flat_shape)
    span = math.gcd(tok_rows, 16)
    block_count = tok_rows // span

    def to_blocks(values):
        return values.reshape(block_count, span, flat_width).transpose(1, 0, 2)

    rows_in = tuple((to_blocks(values) for values in (factor_re, factor_im, drive_re, drive_im)))
    ones_blocks = jnp.ones((block_count, flat_width), jnp.float32)
    zero_blocks = jnp.zeros((block_count, flat_width), jnp.float32)

    def row_step(carry, row):
        joined = compose(carry, row)
        return (joined, joined)

    block_totals, local = lax.scan(
        row_step, (ones_blocks, zero_blocks, zero_blocks, zero_blocks), rows_in
    )
    ones_row = jnp.ones((flat_width,), jnp.float32)
    zero_row = jnp.zeros((flat_width,), jnp.float32)

    def block_step(carry, row):
        return (compose(carry, row), carry)

    totals, before = lax.scan(block_step, (ones_row, zero_row, zero_row, zero_row), block_totals)
    carried = prefix(totals, "sp", compose, (ones_row, zero_row, zero_row, zero_row))
    start_re, start_im = (carried[2], carried[3])
    enter_re = before[0] * start_re[None] - before[1] * start_im[None] + before[2]
    enter_im = before[0] * start_im[None] + before[1] * start_re[None] + before[3]
    state_real = local[2] + local[0] * enter_re[None] - local[1] * enter_im[None]
    state_imaginary = local[3] + local[0] * enter_im[None] + local[1] * enter_re[None]
    group_layout_shape = (tok_rows, group_count, state_size)
    state_real = state_real.transpose(1, 0, 2).reshape(group_layout_shape)
    state_imaginary = state_imaginary.transpose(1, 0, 2).reshape(group_layout_shape)
    result = (
        jnp.einsum("hsv,jhv->jhs", output_real, state_real, precision=upper_limit)
        - jnp.einsum("hsv,jhv->jhs", output_imaginary, state_imaginary, precision=upper_limit)
        + skip.reshape(group_count, group_width)[None] * inputs
    )
    return result.reshape(tok_rows, group_count * group_width).astype(jnp.bfloat16)


def attention_branch(queries, keys_local, values_local, mix_weight, head_gain):
    tok_rows = queries.shape[0]
    head_count = mix_weight.shape[0]
    head_dim = queries.shape[1] // (2 * head_count)
    value_dim = values_local.shape[1] // head_count
    scale = head_dim ** (-0.5)
    first_pos = lax.axis_index("sp") * tok_rows
    query_pos = first_pos + jnp.arange(tok_rows, dtype=jnp.int32)
    query_heads = queries.reshape(tok_rows, head_count, 2, head_dim)
    initial = (
        jnp.full((head_count, 2, tok_rows), -1e30, jnp.float32),
        jnp.zeros((head_count, 2, tok_rows), jnp.float32),
        jnp.zeros((head_count, 2, tok_rows, value_dim), jnp.float32),
    )
    key_piece = lax.all_gather(keys_local, "sp", axis=0, tiled=True)
    value_piece = lax.all_gather(values_local, "sp", axis=0, tiled=True)
    count = key_piece.shape[0]
    block = math.gcd(count, 512)

    def one_block(index, inner):
        run_max, run_total, run_accum = inner
        offset = index * block
        key_block = lax.dynamic_slice_in_dim(key_piece, offset, block, 0).reshape(
            block, head_count, 2, head_dim
        )
        value_block = lax.dynamic_slice_in_dim(value_piece, offset, block, 0).reshape(
            block, head_count, value_dim
        )
        key_pos = offset + jnp.arange(block, dtype=jnp.int32)
        scores = (
            jnp.einsum(
                "qhmd,khmd->hmqk", query_heads, key_block, preferred_element_type=jnp.float32
            )
            * scale
        )
        allowed = key_pos[None, :] <= query_pos[:, None]
        masked = jnp.where(allowed, scores, -1e30)
        new_max = jnp.maximum(run_max, jnp.max(masked, axis=-1))
        weights = jnp.where(allowed, jnp.exp(masked - new_max[..., None]), 0.0)
        rescale = jnp.exp(run_max - new_max)
        new_total = run_total * rescale + jnp.sum(weights, axis=-1)
        product = jnp.einsum(
            "hmqk,khd->hmqd",
            weights.astype(jnp.bfloat16),
            value_block,
            preferred_element_type=jnp.float32,
        )
        return (new_max, new_total, run_accum * rescale[..., None] + product)

    def visit(inner):
        return lax.fori_loop(0, count // block, one_block, inner)

    def keep_carry(inner):
        return inner

    maxima, totals, accum = lax.cond(
        jnp.int32(0) <= first_pos + tok_rows - 1, visit, keep_carry, initial
    )
    log_totals = maxima + jnp.log(totals)
    head_raw = (
        accum[:, 0] / totals[:, 0, :, None]
        - mix_weight[:, None, None] * accum[:, 1] / totals[:, 1, :, None]
    )
    normed_heads = (
        head_raw
        * lax.rsqrt(jnp.mean(head_raw * head_raw, axis=-1, keepdims=True) + 1e-05)
        * head_gain
    )
    attn_out = (
        normed_heads.transpose(1, 0, 2)
        .reshape(tok_rows, head_count * value_dim)
        .astype(jnp.bfloat16)
    )
    return (attn_out, log_totals)


def per_device(
    tokens,
    norm_gain,
    w_state_in,
    w_query,
    w_key,
    w_value,
    decay_re,
    decay_im,
    log_step,
    decay_shift,
    in_re,
    in_im,
    output_real,
    output_imaginary,
    skip,
    mix_weight,
    head_gain,
    w_out_state,
    w_out_attn,
):
    whole = lax.all_gather(tokens, "tp", axis=2, tiled=True)[0]
    floats = whole.astype(jnp.float32)
    normed = (
        floats * lax.rsqrt(jnp.mean(floats * floats, axis=-1, keepdims=True) + 1e-06) * norm_gain
    ).astype(jnp.bfloat16)
    pieces = (
        lax.all_gather(w_state_in, ("sp", "fs"), axis=0, tiled=True),
        lax.all_gather(w_query, ("sp", "fs"), axis=0, tiled=True),
        lax.all_gather(w_key, ("sp", "fs"), axis=0, tiled=True),
        lax.all_gather(w_value, ("sp", "fs"), axis=0, tiled=True),
    )
    sums = tuple((jnp.dot(normed, piece, preferred_element_type=jnp.float32) for piece in pieces))
    state_in = sums[0].astype(jnp.bfloat16)
    queries = sums[1].astype(jnp.bfloat16)
    keys_local = sums[2].astype(jnp.bfloat16)
    values_local = sums[3].astype(jnp.bfloat16)
    attn_out, log_totals = attention_branch(
        queries, keys_local, values_local, mix_weight, head_gain
    )
    state_out = state_branch(
        state_in,
        decay_re,
        decay_im,
        log_step,
        decay_shift,
        in_re,
        in_im,
        output_real,
        output_imaginary,
        skip,
    )
    summed = lax.psum_scatter(
        (
            jnp.dot(state_out, w_out_state, preferred_element_type=jnp.float32)
            + jnp.dot(attn_out, w_out_attn, preferred_element_type=jnp.float32)
        ).astype(jnp.bfloat16),
        "tp",
        scatter_dimension=0,
        tiled=True,
    )
    return (summed[None], log_totals[None])


def nt_dot(a, b):
    return lax.dot_general(a, b, (((1,), (1,)), ((), ())), preferred_element_type=jnp.float32)


def split_pair(x):
    high = x.astype(jnp.bfloat16)
    low = (x - high.astype(jnp.float32)).astype(jnp.bfloat16)
    return (high, low)


def small_expm1(x):
    total = jnp.ones_like(x)
    for n in range(9, 1, -1):
        total = 1.0 + total * x * (1.0 / n)
    return total * x


def fused_kernel(
    sizes,
    tok_ref,
    gain_ref,
    ws_ref,
    wq_ref,
    wk_ref,
    wv_ref,
    dre_ref,
    dim_ref,
    logstep_ref,
    shift_ref,
    inre_ref,
    inim_ref,
    outre_ref,
    outim_ref,
    skip_ref,
    mix_ref,
    hgain_ref,
    wos_ref,
    woa_ref,
    mixed_ref,
    logt_ref,
    stat_send,
    stat_recv,
    nbuf,
    xbuf,
    wbuf,
    pbuf,
    rbuf,
    fin,
    shsend,
    shbuf,
    inbuf,
    outbuf,
    coef,
    etab,
    bcat,
    ccat,
    srow,
    yacc,
    wts,
    stb,
    atb,
    sto,
    ato,
    ltb,
    lto,
    wo,
    acc,
    poutb,
    precb,
    loc_sem,
    wo_sem,
    w_loc,
    stat_sem,
    tok_send,
    tok_recv,
    fwd_send,
    wx_send,
    wx_recv,
    wy_send,
    wy_recv,
    dx_send,
    dx_recv,
    dy_send,
    dy_recv,
    z_send,
    zr_recv,
    zl_recv,
    sh_send,
    sh_recv,
    st_send,
    st_recv,
    at_send,
    at_recv,
    lt_send,
    lt_recv,
    p_send,
    p_recv,
):
    NS, NT, L, D, CW = sizes
    KW = D // NS
    FW = D // NT
    NB = NS // NT
    HC = CW // NS
    SEQ = NS * L
    G = HC // 16
    MESH = pl.DeviceIdType.MESH
    s, f, c = (lax.axis_index("sp"), lax.axis_index("fs"), lax.axis_index("tp"))
    fx = f + 1 - 2 * lax.rem(f, 2)
    fy = lax.rem(f + 2, 4)
    fd = 3 - f
    partner = {"tp": 1 - c}
    owner = s // NB

    def remote(src, dst, send, recv, where):
        return pltpu.make_async_remote_copy(
            src_ref=src, dst_ref=dst, send_sem=send, recv_sem=recv, device_id=where, device_id_type=MESH
        )

    g0 = pl.multiple_of(s * G, G)
    own_w = [
        pltpu.make_async_copy(ref, wbuf.at[m, f], w_loc.at[m])
        for m, ref in enumerate((ws_ref, wq_ref, wk_ref, wv_ref))
    ]
    for copy in own_w:
        copy.start()
    own_p = [
        pltpu.make_async_copy(ref.at[pl.ds(g0, G)], dst, loc_sem.at[i])
        for i, (ref, dst) in enumerate(
            (
                (inre_ref, inbuf.at[0]),
                (inim_ref, inbuf.at[1]),
                (outre_ref, outbuf.at[0]),
                (outim_ref, outbuf.at[1]),
            )
        )
    ]
    for copy in own_p:
        copy.start()
    big = [pltpu.make_async_copy(ref, wo.at[i], wo_sem.at[i]) for i, ref in enumerate((wos_ref, woa_ref))]
    for copy in big:
        copy.start()

    barrier = pltpu.get_barrier_semaphore()
    pl.semaphore_signal(barrier, inc=1, device_id={"fs": fx}, device_id_type=MESH)
    pl.semaphore_signal(barrier, inc=1, device_id={"fs": fy}, device_id_type=MESH)
    pl.semaphore_signal(barrier, inc=1, device_id=partner, device_id_type=MESH)
    for k in range(1, NS):
        pl.semaphore_signal(barrier, inc=1, device_id={"sp": lax.rem(s + k, NS)}, device_id_type=MESH)
    pl.semaphore_wait(barrier, 2 + NS)

    def own_x(m):
        return remote(wbuf.at[m, f], wbuf.at[m, f], wx_send.at[m], wx_recv.at[m], {"fs": fx})

    def own_y(m):
        return remote(wbuf.at[m, f], wbuf.at[m, f], wy_send.at[m], wy_recv.at[m], {"fs": fy})

    half = wbuf.shape[2] // 2

    def fwd_y(m):
        part = wbuf.at[m, fx, pl.ds(0, half)]
        return remote(part, part, dy_send.at[m], dy_recv.at[m], {"fs": fy})

    def fwd_x(m):
        part = wbuf.at[m, fy, pl.ds(half, half)]
        return remote(part, part, dx_send.at[m], dx_recv.at[m], {"fs": fx})

    tokens = tok_ref[0].astype(jnp.float32)
    square = jnp.sum(tokens * tokens, axis=1, keepdims=True)
    stat_send[...] = jnp.broadcast_to(square, (L, 128))
    stat = remote(stat_send, stat_recv, stat_sem.at[0], stat_sem.at[1], partner)
    stat.start()
    for m in range(4):
        own_w[m].wait()
    for m in range(2):
        own_x(m).start()
        own_y(m).start()
    for d in range(NS):
        shsend[d] = shift_ref[0, d * G : (d + 1) * G, :]
    for k in range(1, NS):
        d = lax.rem(s + k, NS)
        remote(shsend.at[d], shbuf.at[s], sh_send.at[d], sh_recv.at[s], {"sp": d}).start()
    shbuf[s] = shsend[s]
    stat.wait()
    mean = (square + stat_recv[:, 0:1]) * (1.0 / D)
    gain = gain_ref[:, pl.ds(pl.multiple_of(c * FW, FW), FW)]
    normed = (tok_ref[0].astype(jnp.float32) * lax.rsqrt(mean + 1e-06) * gain).astype(jnp.bfloat16)

    def tok_copy(i):
        return remote(
            nbuf.at[i], xbuf.at[s], tok_send.at[i], tok_recv.at[s], {"sp": c * NB + i}
        )

    for i in range(NB):
        nbuf[i] = normed[:, i * KW : (i + 1) * KW]
    for i in range(NB):
        @pl.when(c * NB + i != s)
        def _():
            tok_copy(i).start()

        @pl.when(c * NB + i == s)
        def _():
            xbuf[s] = nbuf[i]

    def tok_forward(q):
        return remote(xbuf.at[q], xbuf.at[q], fwd_send.at[q], tok_recv.at[q], partner)

    def tok_arrival(q):
        return remote(xbuf.at[q], xbuf.at[q], fwd_send.at[q], tok_recv.at[q], partner)

    re16 = dre_ref[pl.ds(g0, G), :]
    im16 = dim_ref[pl.ds(g0, G), :]
    re16 = jnp.concatenate([re16, re16], axis=1)
    im16 = jnp.concatenate([im16, im16], axis=1)
    numer_re = small_expm1(re16) * jnp.cos(im16) - 2.0 * jnp.sin(0.5 * im16) ** 2
    numer_im = jnp.exp(re16) * jnp.sin(im16)
    modulus = re16 * re16 + im16 * im16
    coef[0] = re16
    coef[1] = im16
    coef[2] = (numer_re * re16 + numer_im * im16) / modulus
    coef[3] = (numer_im * re16 - numer_re * im16) / modulus
    for copy in own_p:
        copy.wait()
    lane = lax.broadcasted_iota(jnp.int32, (128, 16), 0)
    chan = lax.broadcasted_iota(jnp.int32, (128, 16), 1)
    steps = lax.broadcasted_iota(jnp.int32, (L, 128), 0).astype(jnp.float32) + 1.0
    sel_hi = lax.broadcasted_iota(jnp.int32, (128, 16), 0)

    def table(g, carry):
        zr = coef[0, pl.ds(g, 1), :]
        zi = coef[1, pl.ds(g, 1), :]
        step = jnp.exp(jnp.full((1, 128), logstep_ref[g0 + g], jnp.float32))
        cr = coef[2, pl.ds(g, 1), :] * step
        ci = coef[3, pl.ds(g, 1), :] * step
        angle = steps * zi
        cosine, sine = (jnp.cos(angle), jnp.sin(angle))
        shrink = jnp.exp(steps * zr)
        grow = jnp.exp(-(steps * zr))
        etab[0, g] = grow * (cosine * cr + sine * ci)
        etab[1, g] = grow * (cosine * ci - sine * cr)
        etab[2, g] = shrink * cosine
        etab[3, g] = shrink * sine
        pick = (lane == lax.rem(g, 8) * 16 + chan).astype(jnp.bfloat16)
        ir, ii = (inbuf[0, g], inbuf[1, g])
        raw = jnp.concatenate([ir, ii, -ii, ir], axis=1)
        hi, lo = split_pair(raw)
        bcat[g] = jnp.concatenate(
            [
                jnp.dot(pick, hi, preferred_element_type=jnp.float32).astype(jnp.bfloat16),
                jnp.dot(pick, lo, preferred_element_type=jnp.float32).astype(jnp.bfloat16),
            ],
            axis=0,
        )
        cr_, ci_ = (outbuf[0, g], outbuf[1, g])
        rawc = jnp.concatenate([cr_, -ci_, -ci_, -cr_], axis=1)
        hi, lo = split_pair(rawc)
        ccat[g] = jnp.concatenate(
            [
                jnp.dot(pick, hi, preferred_element_type=jnp.float32).astype(jnp.bfloat16),
                jnp.dot(pick, lo, preferred_element_type=jnp.float32).astype(jnp.bfloat16),
            ],
            axis=0,
        )
        return carry

    lax.fori_loop(0, G, table, 0)
    for k in range(1, NS):
        q = lax.rem(s + k, NS)
        remote(shsend.at[q], shbuf.at[q], sh_send.at[q], sh_recv.at[q], {"sp": q}).wait_recv()
    row_i = lax.broadcasted_iota(jnp.int32, (L, L), 0)
    col_i = lax.broadcasted_iota(jnp.int32, (L, L), 1)
    upper = (row_i <= col_i).astype(jnp.float32)
    for k in range(NS):
        srow[k] = jnp.dot(
            shbuf[k], upper, precision=lax.Precision.HIGHEST, preferred_element_type=jnp.float32
        )

    for k in range(NS):
        q = lax.rem(s + k, NS)

        @pl.when(c == owner)
        def _():
            @pl.when(q != s)
            def _():
                tok_arrival(q).wait_recv()

            tok_forward(q).start()

        @pl.when(c != owner)
        def _():
            tok_arrival(q).wait_recv()

    def z_right(m, d):
        return remote(pbuf.at[m, d], rbuf.at[0, m, d], z_send.at[m, d], zr_recv.at[m, d], {"sp": lax.rem(s + 1, NS)})

    def z_left(m, d):
        return remote(
            pbuf.at[m, d], rbuf.at[1, m, d], z_send.at[m, d], zl_recv.at[m, d], {"sp": lax.rem(s + NS - 1, NS)}
        )

    def hop_right(m, k):
        d = NS - 1 - k

        @pl.when(d > s)
        def _():
            z_right(m, d).wait_recv()
            pbuf[m, d] = (pbuf[m, d].astype(jnp.float32) + rbuf[0, m, d].astype(jnp.float32)).astype(jnp.bfloat16)
            z_right(m, d).start()

    def hop_left(m, d):
        @pl.when(d < s)
        def _():
            z_left(m, d).wait_recv()
            pbuf[m, d] = (pbuf[m, d].astype(jnp.float32) + rbuf[1, m, d].astype(jnp.float32)).astype(jnp.bfloat16)
            z_left(m, d).start()

    def each(hop, m):
        def one(k, carry):
            hop(m, k)
            return carry

        lax.fori_loop(0, NS, one, 0)

    def relay(m):
        @pl.when(jnp.logical_and(s > 0, s < NS // 2))
        def _():
            each(hop_right, m)
            each(hop_left, m)

        @pl.when(jnp.logical_and(s >= NS // 2, s < NS - 1))
        def _():
            each(hop_left, m)
            each(hop_right, m)


    def project(m, carry):
        own_x(m).wait_recv()
        own_y(m).wait_recv()
        fwd_y(m).start()
        fwd_x(m).start()

        @pl.when(m < 2)
        def _():
            own_x(m + 2).start()
            own_y(m + 2).start()

        @pl.when(m > 0)
        def _():
            relay(m - 1)

        diag_y = wbuf.at[m, fd, pl.ds(0, half)]
        diag_x = wbuf.at[m, fd, pl.ds(half, half)]
        remote(diag_y, diag_y, dy_send.at[m], dy_recv.at[m], {"fs": fy}).wait_recv()
        remote(diag_x, diag_x, dx_send.at[m], dx_recv.at[m], {"fs": fx}).wait_recv()

        def block(k, inner):
            d = jnp.where(s < NS // 2, NS - 1 - k, k)
            columns = pl.ds(pl.multiple_of(d * HC, HC), HC)
            lhs = xbuf[...].reshape(SEQ, KW)
            rhs = wbuf[m, :, :, columns].reshape(KW, HC)
            part = jnp.dot(lhs, rhs, preferred_element_type=jnp.float32).astype(jnp.bfloat16)

            pbuf[m, d] = part

            @pl.when(jnp.logical_and(s == 0, d > 0))
            def _():
                z_right(m, d).start()

            @pl.when(jnp.logical_and(s == NS - 1, d < NS - 1))
            def _():
                z_left(m, d).start()

            return inner

        return lax.fori_loop(0, NS, block, carry)

    def finish(m):
        @pl.when(s > 0)
        def _():
            z_right(m, s).wait_recv()

        @pl.when(s < NS - 1)
        def _():
            z_left(m, s).wait_recv()

        own = pbuf[m, s].astype(jnp.float32)

        @pl.when(s == 0)
        def _():
            fin[m] = (own + rbuf[1, m, s].astype(jnp.float32)).astype(jnp.bfloat16)

        @pl.when(s == NS - 1)
        def _():
            fin[m] = (own + rbuf[0, m, s].astype(jnp.float32)).astype(jnp.bfloat16)

        @pl.when(jnp.logical_and(s > 0, s < NS - 1))
        def _():
            fin[m] = (own + rbuf[0, m, s].astype(jnp.float32) + rbuf[1, m, s].astype(jnp.float32)).astype(jnp.bfloat16)

    lax.fori_loop(0, 3, project, 0)

    finish(0)
    sign = jnp.where(lax.broadcasted_iota(jnp.int32, (8, 128), 1) < 64, -1.0, 1.0)
    lower = row_i >= col_i

    def lane_block(b, carry):
        lanes = pl.ds(pl.multiple_of(b * 128, 128), 128)
        u = fin[0, :, lanes]
        uu = jnp.concatenate([u, u], axis=1)
        yacc[...] = jnp.zeros_like(yacc)

        def group(g8, inner):
            g = b * 8 + g8
            drives = jnp.dot(uu, bcat[g], preferred_element_type=jnp.float32)
            h = jnp.zeros((1, 128), jnp.float32)
            er, ei, fr, fi = (etab[0, g], etab[1, g], etab[2, g], etab[3, g])
            for k in range(NS):
                d = drives[k * L : (k + 1) * L]
                x = er * d[:, :128] + ei * d[:, 128:]
                xh, xl = split_pair(x)
                xx = jnp.concatenate([xh, xl], axis=1)
                rhs = jnp.concatenate([xx, xx], axis=0)
                sr = jnp.broadcast_to(srow[k, pl.ds(g, 1), :], (L, L))
                sc = sr.T
                mask = jnp.where(lower, jnp.exp(jnp.minimum(sc - sr, 0.0)), 0.0)
                mh, ml = split_pair(mask)
                w2 = jnp.dot(
                    jnp.concatenate([mh, ml], axis=1), rhs, preferred_element_type=jnp.float32
                )
                q = w2[:, :128] + w2[:, 128:] + jnp.exp(sc) * h
                p1 = q * fr
                p2 = q * fi
                tail = p1[L - 8 :] + sign * pltpu.roll(p2[L - 8 :], 64, 1)
                h = tail[7:8]
                ph, plow = split_pair(jnp.concatenate([p1, p2], axis=1))
                y2 = nt_dot(ph, ccat[g]) + nt_dot(plow, ccat[g])
                yacc[k * L : (k + 1) * L, :] += y2[:, :128] + y2[:, 128:]
            return inner

        lax.fori_loop(0, 8, group, 0)
        direct = skip_ref[:, pl.ds(pl.multiple_of(s * HC + b * 128, 128), 128)]
        out = (yacc[...] + direct * u.astype(jnp.float32)).astype(jnp.bfloat16)
        for k in range(NS):
            stb[k, :, lanes] = out[k * L : (k + 1) * L]
        return carry

    lax.fori_loop(0, HC // 128, lane_block, 0)

    lax.fori_loop(3, 4, project, 0)

    def st_copy(d):
        return remote(stb.at[d], sto.at[s], st_send.at[d], st_recv.at[s], {"sp": d})

    def at_copy(d):
        return remote(atb.at[d], ato.at[s], at_send.at[d], at_recv.at[s], {"sp": d})

    def lt_copy(d):
        return remote(ltb.at[d], lto.at[s], lt_send.at[d], lt_recv.at[s], {"sp": d})

    for k in range(1, NS):
        st_copy(lax.rem(s + k, NS)).start()
    sto[s] = stb[s]

    hd = HC // 2
    relay(3)
    finish(1)
    finish(2)
    lam = mix_ref[s]
    totals = []
    for i in range(NS):
        width = (i + 1) * L
        for m in range(2):
            sc = nt_dot(
                fin[1, i * L : (i + 1) * L, m * hd : (m + 1) * hd], fin[2, 0:width, m * hd : (m + 1) * hd]
            ) * (hd ** (-0.5))
            qpos = lax.broadcasted_iota(jnp.int32, (L, width), 0) + i * L
            kpos = lax.broadcasted_iota(jnp.int32, (L, width), 1)
            allowed = kpos <= qpos
            sc = jnp.where(allowed, sc, -1e30)
            top = jnp.max(sc, axis=1, keepdims=True)
            weights = jnp.where(allowed, jnp.exp(sc - top), 0.0)
            total = jnp.sum(weights, axis=1, keepdims=True)
            wts[m, i * L : (i + 1) * L, 0:width] = weights.astype(jnp.bfloat16)
            totals.append(1.0 / total)
            logs = jnp.broadcast_to(top + jnp.log(total), (L, L)).T
            ltb[i, m : m + 1, :] = logs[0:1]
    for k in range(1, NS):
        lt_copy(lax.rem(s + k, NS)).start()
    lto[s] = ltb[s]
    finish(3)
    for i in range(NS):
        width = (i + 1) * L
        heads = [
            jnp.dot(
                wts[m, i * L : (i + 1) * L, 0:width], fin[3, 0:width, :], preferred_element_type=jnp.float32
            )
            * totals[2 * i + m]
            for m in range(2)
        ]
        raw = heads[0] - lam * heads[1]
        scale = lax.rsqrt(jnp.mean(raw * raw, axis=1, keepdims=True) + 1e-05)
        atb[i] = (raw * scale * hgain_ref[...]).astype(jnp.bfloat16)

    for k in range(1, NS):
        d = lax.rem(s + k, NS)
        at_copy(d).start()
    ato[s] = atb[s]

    for copy in big:
        copy.wait()
    for k in range(1, NS):
        q = lax.rem(s + k, NS)
        remote(stb.at[q], sto.at[q], st_send.at[q], st_recv.at[q], {"sp": q}).wait_recv()
    tiles = poutb.shape[0]
    width = D // tiles
    st_lhs = jnp.concatenate([sto[q] for q in range(NS)], axis=1)

    def state_tile(n, carry):
        columns = pl.ds(pl.multiple_of(n * width, width), width)
        acc[:, columns] = jnp.dot(st_lhs, wo[0, :, columns], preferred_element_type=jnp.float32)
        return carry

    lax.fori_loop(0, tiles, state_tile, 0)
    for k in range(1, NS):
        q = lax.rem(s + k, NS)
        remote(atb.at[q], ato.at[q], at_send.at[q], at_recv.at[q], {"sp": q}).wait_recv()
    at_lhs = jnp.concatenate([ato[q] for q in range(NS)], axis=1)
    rows = L // NT
    mine = pl.ds(pl.multiple_of(c * rows, rows), rows)

    def p_copy(n):
        theirs = pl.ds(pl.multiple_of((1 - c) * rows, rows), rows)
        return remote(poutb.at[n, theirs], precb.at[n], p_send.at[n], p_recv.at[n], partner)

    def attn_tile(n, carry):
        columns = pl.ds(pl.multiple_of(n * width, width), width)
        part = acc[:, columns] + jnp.dot(at_lhs, wo[1, :, columns], preferred_element_type=jnp.float32)
        poutb[n] = part.astype(jnp.bfloat16)
        p_copy(n).start()
        return carry

    lax.fori_loop(0, tiles, attn_tile, 0)

    def last_tile(n, carry):
        columns = pl.ds(pl.multiple_of(n * width, width), width)
        p_copy(n).wait()
        mixed_ref[0, :, columns] = (
            poutb[n, mine, :].astype(jnp.float32) + precb[n].astype(jnp.float32)
        ).astype(jnp.bfloat16)
        return carry

    lax.fori_loop(0, tiles, last_tile, 0)
    for k in range(1, NS):
        q = lax.rem(s + k, NS)
        remote(ltb.at[q], lto.at[q], lt_send.at[q], lt_recv.at[q], {"sp": q}).wait_recv()
    logt_ref[0] = lto[...]

    for m in range(4):
        own_x(m).wait_send()
        own_y(m).wait_send()
        fwd_x(m).wait_send()
        fwd_y(m).wait_send()
        for k in range(1, NS):
            z_right(m, lax.rem(s + k, NS)).wait_send()
    for k in range(1, NS):
        d = lax.rem(s + k, NS)
        remote(shsend.at[d], shbuf.at[s], sh_send.at[d], sh_recv.at[s], {"sp": d}).wait_send()
        st_copy(d).wait_send()
        at_copy(d).wait_send()
        lt_copy(d).wait_send()
    for i in range(NB):
        @pl.when(c * NB + i != s)
        def _():
            tok_copy(i).wait_send()

    @pl.when(c == owner)
    def _():
        for q in range(NS):
            tok_forward(q).wait_send()


def fused_device(sizes, *args):
    (tokens, norm_gain, ws, wq, wk, wv, dre, dim, logstep, shift, inre, inim, outre, outim, skip, mix, hgain, wos, woa) = args
    NS, NT, L, D, CW = sizes
    KW, HC = (D // NS, CW // NS)
    SEQ, G, NB, NF = (NS * L, HC // 16, NS // NT, 4)
    tiles = 8
    bf, f32 = (jnp.bfloat16, jnp.float32)
    V = pltpu.VMEM
    DMA = pltpu.SemaphoreType.DMA
    vmem = pl.BlockSpec(memory_space=pltpu.VMEM)
    smem = pl.BlockSpec(memory_space=pltpu.SMEM)
    hbm = pl.BlockSpec(memory_space=pl.ANY)
    scratch = [
        V((L, 128), f32),
        V((L, 128), f32),
        V((NB, L, KW), bf),
        V((NS, L, KW), bf),
        V((4, NF, ws.shape[0], CW), bf),
        V((4, NS, SEQ, HC), bf),
        V((2, 4, NS, SEQ, HC), bf),
        V((4, SEQ, HC), bf),
        V((NS, G, L), f32),
        V((NS, G, L), f32),
        V((2, G, 16, 64), f32),
        V((2, G, 16, 64), f32),
        V((4, G, 128), f32),
        V((4, G, L, 128), f32),
        V((G, 256, 256), bf),
        V((G, 256, 256), bf),
        V((NS, G, L), f32),
        V((SEQ, 128), f32),
        V((2, SEQ, SEQ), bf),
        V((NS, L, HC), bf),
        V((NS, L, HC), bf),
        V((NS, L, HC), bf),
        V((NS, L, HC), bf),
        V((NS, 2, L), f32),
        V((NS, 2, L), f32),
        V((2, CW, D), bf),
        V((L, D), f32),
        V((tiles, L, D // tiles), bf),
        V((tiles, L // NT, D // tiles), bf),
        DMA((4,)),
        DMA((2,)),
        DMA((4,)),
        DMA((2,)),
        DMA((NB,)),
        DMA((NS,)),
        DMA((NS,)),
    ]
    scratch += [DMA((4,))] * 8
    scratch += [DMA((4, NS))] * 3
    scratch += [DMA((NS,))] * 8
    scratch += [DMA((tiles,))] * 2
    call = pl.pallas_call(
        functools.partial(fused_kernel, sizes),
        out_shape=(
            jax.ShapeDtypeStruct((1, L // NT, D), bf),
            jax.ShapeDtypeStruct((1, NS, 2, L), f32),
        ),
        in_specs=[vmem, vmem, hbm, hbm, hbm, hbm, vmem, vmem, smem, vmem, hbm, hbm, hbm, hbm, vmem, smem, vmem, hbm, hbm],
        out_specs=(vmem, vmem),
        scratch_shapes=scratch,
        compiler_params=pltpu.CompilerParams(
            collective_id=0, has_side_effects=True, vmem_limit_bytes=67043328
        ),
    )
    return call(
        tokens, norm_gain.reshape(1, -1), ws, wq, wk, wv, dre, dim, logstep, shift,
        inre.transpose(0, 2, 1), inim.transpose(0, 2, 1), outre, outim,
        skip.reshape(1, -1), mix, hgain.reshape(1, -1), wos, woa,
    )


def choose_device(sp, fs, tp, *args):
    tokens, ws, dre, inre, mix = (args[0], args[2], args[6], args[10], args[15])
    L, D = (tokens.shape[1], ws.shape[0] * sp * fs)
    CW = ws.shape[1]
    fits = (
        fs == 4
        and tp == 2
        and sp % tp == 0
        and mix.shape[0] == sp
        and L == 128
        and CW == sp * 256
        and dre.shape == (sp * 16, 64)
        and inre.shape[2] == 16
        and D % (sp * 128) == 0
    )
    if fits:
        return fused_device((sp, tp, L, D, CW), *args)
    return per_device(*args)


def solution(mesh):
    in_specs = (
        P("fs", "sp", "tp"),
        P(),
        P(("sp", "fs"), "tp"),
        P(("sp", "fs"), "tp"),
        P(("sp", "fs"), "tp"),
        P(("sp", "fs"), "tp"),
        P("tp", None),
        P("tp", None),
        P("tp"),
        P("fs", "tp", "sp"),
        P("tp", None, None),
        P("tp", None, None),
        P("tp", None, None),
        P("tp", None, None),
        P("tp"),
        P("tp"),
        P(),
        P("tp", None),
        P("tp", None),
    )
    out_specs = (P("fs", ("sp", "tp"), None), P("fs", "tp", None, "sp"))
    body = functools.partial(choose_device, mesh.shape["sp"], mesh.shape["fs"], mesh.shape["tp"])
    return jax.shard_map(
        body, mesh=mesh, in_specs=in_specs, out_specs=out_specs, check_vma=False
    )
```
